32 devices in a mesh: sp: 4 (over z), fs: 4 (over y, x), tp: 2 (over core).
Axes of the slice: x: 2, y: 2, z: 4, core: 2. Of those that a mesh axis runs over, the one named last changes fastest.
Arguments:
- layer_entering_vectors: bfloat16 [4, 1024, 2048], P('fs', ('sp', 'tp')), may hold values from -6 to 6
- entering_rms_coefficients: float32 [2048], replicated, may hold values from 0.1 to 1.9
- question_projection: bfloat16 [2048, 1536], P('fs', 'tp'), may hold values from -0.125 to 0.125
- compressing_projection: bfloat16 [2048, 256], P('fs'), may hold values from -0.125 to 0.125
- spinning_address_projection: bfloat16 [2048, 32], P('fs'), may hold values from -0.125 to 0.125
- compact_rms_coefficients: float32 [256], replicated, may hold values from 0.1 to 1.9
- compact_to_plain_address: bfloat16 [256, 1024], P(None, 'tp'), may hold values from -0.375 to 0.375
- compact_to_content: bfloat16 [256, 1024], P(None, 'tp'), may hold values from -0.375 to 0.375
- question_rms_coefficients: float32 [96], replicated, may hold values from 0.7 to 6
- address_rms_coefficients: float32 [96], replicated, may hold values from 0.7 to 6
- acceptance_projection: bfloat16 [2048, 1024], P('fs', 'tp'), may hold values from -0.125 to 0.125
- state_address_projection: bfloat16 [2048, 1024], P('fs', 'tp'), may hold values from -0.125 to 0.125
- state_content_projection: bfloat16 [2048, 1024], P('fs', 'tp'), may hold values from -0.125 to 0.125
- fading_first_lowrank: bfloat16 [2048, 128], replicated, may hold values from -0.125 to 0.125
- fading_second_lowrank: bfloat16 [128, 1024], P(None, 'tp'), may hold values from -0.375 to 0.375
- fading_channel_bias: float32 [1024], P('tp'), may hold values from -20 to -2
- fading_speed_multiplier: float32 [4, 16, 1024], P('fs', 'tp', 'sp'), may hold values from 0.5 to 2, as said below
- fading_extra_exponent: float32 [4, 16, 1024], P('fs', 'tp', 'sp'), may hold values from -0.7 to 0
- adaptation_first_lowrank: bfloat16 [2048, 128], replicated, may hold values from -0.125 to 0.125
- adaptation_second_lowrank: bfloat16 [128, 1024], P(None, 'tp'), may hold values from -0.5 to 0.5
- adaptation_channel_bias: float32 [1024], P('tp'), may hold values from -12 to -1
- present_token_coefficients: float32 [16, 64], P('tp'), may hold values from -1.5 to 1.5
- branch_rms_coefficients: float32 [1024], P('tp'), may hold values from 0.1 to 1.9
- softmax_merge_projection: bfloat16 [1024, 2048], P('tp', 'fs'), may hold values from -0.1875 to 0.1875
- state_merge_projection: bfloat16 [1024, 2048], P('tp', 'fs'), may hold values from -0.1875 to 0.1875
Outputs:
- mixed: bfloat16 [4, 1024, 2048], P('fs', ('sp', 'tp'))
- log_total: float32 [4, 16, 1024], P('fs', 'tp', 'sp')
The draws below stay inside these ranges and needn't reach their ends.
Inputs may be any that keep to these rules, and one draw needn't show every extreme that they name: `fading_speed_multiplier`: constant over aligned blocks of 256 positions.
All inputs are finite; a program needn't handle non-finite values.
Results may differ from the reference program's by a relative error of at most 0.015.
Values may be sent and summed in bfloat16 or wider, within the bound.
A program may use at most 128 MiB of HBM per device.

```python
import math
import jax
import jax.numpy as jnp
from jax import lax

D = 2048
MHEADS = 16
NOPE = 64
ROPE = 32
VHEAD = 64
KVLAT = 256
STATE_BRANCHES = 16
BRANCH_CHANNELS = 64
DLORA = 128
ALORA = 128
TOK_DEV = 256
SEQS = 4
TOKEN_SPAN = 1024
N_TP = 2


def draw_gain_common(key):
    return jax.random.uniform(key, (NOPE + ROPE,), jnp.float32, 0.7, 1.3)


def draw_question_rms_coefficients(key, part):
    return draw_gain_common(jax.random.fold_in(key, 11))


def draw_address_rms_coefficients(key, part):
    return draw_gain_common(jax.random.fold_in(key, 12))


def draw_fading_channel_bias(key, part):
    first, second = jax.random.split(jax.random.fold_in(key, 21))
    quick = jax.random.uniform(first, (STATE_BRANCHES,), jnp.float32) < 0.5
    slow_value = jnp.log(0.15 / TOKEN_SPAN) + 0.5
    centre = jnp.where(quick, -3.2, slow_value)
    jitter = jax.random.uniform(second, (STATE_BRANCHES, BRANCH_CHANNELS), jnp.float32, -0.5, 0.5)
    return (centre[:, None] + jitter).reshape(STATE_BRANCHES * BRANCH_CHANNELS)


def draw_adaptation_channel_bias(key, part):
    spread = jax.random.uniform(jax.random.fold_in(key, 31), (STATE_BRANCHES * BRANCH_CHANNELS,), jnp.float32, math.log(8.0), math.log(40.0))
    return spread - math.log(max(TOKEN_SPAN, 256) * 1.0)


def draw_fading_speed_multiplier(key, part):
    blocks = TOKEN_SPAN // TOK_DEV
    values = jnp.exp(jax.random.uniform(jax.random.fold_in(key, 41), (SEQS, STATE_BRANCHES, blocks), jnp.float32, math.log(0.5), math.log(2.0)))
    return jnp.repeat(values, TOK_DEV, axis=2)


def draw_fading_extra_exponent(key, part):
    first, second = jax.random.split(jax.random.fold_in(key, 51))
    stratum = TOKEN_SPAN // 3
    offsets = jax.random.randint(first, (SEQS, 3), 0, stratum, dtype=jnp.int32)
    places = offsets + stratum * jnp.arange(3, dtype=jnp.int32)[None, :]
    strength = jax.random.uniform(second, (SEQS, STATE_BRANCHES, 3), jnp.float32, 0.2, 0.5)
    where_hit = (jnp.arange(TOKEN_SPAN, dtype=jnp.int32)[None, None, None, :] == places[:, None, :, None]).astype(jnp.float32)
    return jnp.sum(jnp.log(1.0 - strength)[..., None] * where_hit, axis=2)


def block_scale(stream_key, shape, shards, smallest, top_value):
    def one(position, parts):
        draws = jax.random.uniform(jax.random.fold_in(jax.random.fold_in(stream_key, 6), position), (parts,), jnp.float32, smallest / len(shards), top_value / len(shards))
        return jnp.repeat(jnp.exp(draws), shape[position] // parts).reshape((-1,) + (1,) * (len(shape) - position - 1))

    loudness = one(*shards[0])
    for cut in shards[1:]:
        loudness = loudness * one(*cut)
    return loudness


def normal_values(key, extent, deviation, reach, pieces=(), held_as=jnp.bfloat16):
    level = block_scale(key, extent, pieces, -0.22, 0.18) if pieces else 1.0
    entries = jax.random.normal(key, extent, jnp.float32) * deviation * level
    return jnp.minimum(jnp.maximum(entries, -reach), reach).astype(held_as)


def setup_inputs(seed: int = 0) -> dict:
    key_list = jax.random.split(jax.random.key(seed), 26)
    return {
        "layer_entering_vectors": normal_values(key_list[0], (SEQS, TOKEN_SPAN, D), 1.0, 6.0, ((0, 4), (1, 8))),
        "entering_rms_coefficients": jnp.clip(1.0 + 0.18 * jax.random.normal(key_list[1], (D,), jnp.float32), 0.1, 1.9),
        "question_projection": normal_values(key_list[2], (D, MHEADS * (NOPE + ROPE)), D ** -0.5, 0.125, ((0, 4), (1, 2))),
        "compressing_projection": normal_values(key_list[3], (D, KVLAT), D ** -0.5, 0.125, ((0, 4),)),
        "spinning_address_projection": normal_values(key_list[4], (D, ROPE), D ** -0.5, 0.125, ((0, 4),)),
        "compact_rms_coefficients": jnp.clip(1.0 + 0.18 * jax.random.normal(key_list[5], (KVLAT,), jnp.float32), 0.1, 1.9),
        "compact_to_plain_address": normal_values(key_list[6], (KVLAT, MHEADS * NOPE), KVLAT ** -0.5, 0.375, ((1, 2),)),
        "compact_to_content": normal_values(key_list[7], (KVLAT, MHEADS * VHEAD), KVLAT ** -0.5, 0.375, ((1, 2),)),
        "question_rms_coefficients": draw_question_rms_coefficients(jax.random.fold_in(key_list[25], 71), 0),
        "address_rms_coefficients": draw_address_rms_coefficients(jax.random.fold_in(key_list[25], 71), 0),
        "acceptance_projection": normal_values(key_list[10], (D, STATE_BRANCHES * BRANCH_CHANNELS), D ** -0.5, 0.125, ((0, 4), (1, 2))),
        "state_address_projection": normal_values(key_list[11], (D, STATE_BRANCHES * BRANCH_CHANNELS), D ** -0.5, 0.125, ((0, 4), (1, 2))),
        "state_content_projection": normal_values(key_list[12], (D, STATE_BRANCHES * BRANCH_CHANNELS), D ** -0.5, 0.125, ((0, 4), (1, 2))),
        "fading_first_lowrank": normal_values(key_list[13], (D, DLORA), D ** -0.5, 0.125),
        "fading_second_lowrank": normal_values(key_list[14], (DLORA, STATE_BRANCHES * BRANCH_CHANNELS), (2 * DLORA) ** -0.5, 0.375, ((1, 2),)),
        "fading_channel_bias": draw_fading_channel_bias(jax.random.fold_in(key_list[25], 71), 0),
        "fading_speed_multiplier": draw_fading_speed_multiplier(jax.random.fold_in(key_list[25], 71), 0),
        "fading_extra_exponent": draw_fading_extra_exponent(jax.random.fold_in(key_list[25], 71), 0),
        "adaptation_first_lowrank": normal_values(key_list[18], (D, ALORA), D ** -0.5, 0.125),
        "adaptation_second_lowrank": normal_values(key_list[19], (ALORA, STATE_BRANCHES * BRANCH_CHANNELS), ALORA ** -0.5, 0.5, ((1, 2),)),
        "adaptation_channel_bias": draw_adaptation_channel_bias(jax.random.fold_in(key_list[25], 71), 0),
        "present_token_coefficients": normal_values(key_list[21], (STATE_BRANCHES, BRANCH_CHANNELS), 0.3, 1.5, ((0, 2),), jnp.float32),
        "branch_rms_coefficients": jnp.clip(1.0 + 0.18 * jax.random.normal(key_list[22], (STATE_BRANCHES * BRANCH_CHANNELS,), jnp.float32), 0.1, 1.9),
        "softmax_merge_projection": normal_values(key_list[23], (MHEADS * VHEAD, D), (MHEADS * VHEAD) ** -0.5, 0.1875, ((0, 2), (1, 4))),
        "state_merge_projection": normal_values(key_list[24], (STATE_BRANCHES * BRANCH_CHANNELS, D), (STATE_BRANCHES * BRANCH_CHANNELS) ** -0.5, 0.1875, ((0, 2), (1, 4))),
    }


norm_epsilon = 1e-06
group_epsilon = 0.00064
highest = lax.Precision.HIGHEST

def rms_rows(values, gain):
    floats = values.astype(jnp.float32)
    return floats * lax.rsqrt(lax.optimization_barrier(jnp.mean(floats * floats, axis=-1, keepdims=True)) + norm_epsilon) * gain

def rotate(values, positions):
    half = values.shape[-1] // 2
    inverse = 10000.0 ** (-jnp.arange(half, dtype=jnp.float32) / half)
    angle = positions.astype(jnp.float32)[:, None] * inverse[None, :]
    cosine = jnp.cos(angle)[:, None, :]
    sine = jnp.sin(angle)[:, None, :]
    first = values[..., :half]
    second = values[..., half:]
    return jnp.concatenate([first * cosine - second * sine, second * cosine + first * sine], axis=-1)

def finish(stacked, gain, positions):
    normed = rms_rows(stacked, gain)
    return jnp.concatenate([normed[..., :NOPE], rotate(normed[..., NOPE:], positions)], axis=-1).astype(jnp.bfloat16)

def matmul(left, right):
    return jnp.dot(left, right, preferred_element_type=jnp.float32)

def recur(state, inputs):
    decay_now, unit_now, learn_now, value_now, key_now, recept_now = inputs
    along = jnp.einsum('hvk,hk->hv', state, unit_now, precision=highest)
    state = state * decay_now[:, None, :] - along[:, :, None] * (unit_now * learn_now)[:, None, :] + value_now[:, :, None] * key_now[:, None, :]
    return (state, jnp.einsum('hvk,hk->hv', state, recept_now, precision=highest))

def solo_stream(entering_tokens_flat, entering_rms_coefficients, question_projection, compressing_projection, spinning_address_projection, compact_rms_coefficients, compact_to_plain_address, compact_to_content, question_rms_coefficients, address_rms_coefficients, acceptance_projection, state_address_projection, state_content_projection, fading_first_lowrank, fading_second_lowrank, fading_channel_bias, fading_speed_multiplier, fading_extra_exponent, adaptation_first_lowrank, adaptation_second_lowrank, adaptation_channel_bias, present_token_coefficients, branch_rms_coefficients, softmax_merge_projection, state_merge_projection):
    positions = jnp.arange(TOKEN_SPAN, dtype=jnp.int32)
    normed = rms_rows(entering_tokens_flat, entering_rms_coefficients).astype(jnp.bfloat16)
    query = matmul(normed, question_projection).astype(jnp.bfloat16).reshape(TOKEN_SPAN, MHEADS, NOPE + ROPE)
    latent = matmul(normed, compressing_projection).astype(jnp.bfloat16)
    rope_key = matmul(normed, spinning_address_projection).astype(jnp.bfloat16)
    latent_normed = rms_rows(latent, compact_rms_coefficients).astype(jnp.bfloat16)
    key_nope = matmul(latent_normed, compact_to_plain_address).astype(jnp.bfloat16).reshape(TOKEN_SPAN, MHEADS, NOPE)
    values_heads = matmul(latent_normed, compact_to_content).astype(jnp.bfloat16).reshape(TOKEN_SPAN, MHEADS, VHEAD)
    key_stack = jnp.concatenate([key_nope, jnp.broadcast_to(rope_key[:, None, :], (TOKEN_SPAN, MHEADS, ROPE))], axis=-1)
    query_ready = finish(query, question_rms_coefficients, positions)
    key_ready = finish(key_stack, address_rms_coefficients, positions)
    scale = (NOPE + ROPE) ** (-0.5)
    keys_wide = key_ready.astype(jnp.float32)
    values_wide = values_heads.astype(jnp.float32)

    def attend(block):
        start = block * TOK_DEV
        query_block = lax.dynamic_slice_in_dim(query_ready, start, TOK_DEV, 0).astype(jnp.float32)
        scores = jnp.einsum('qhd,khd->hqk', query_block, keys_wide) * scale
        allowed = positions[None, :] <= (start + jnp.arange(TOK_DEV, dtype=jnp.int32))[:, None]
        scores = jnp.where(allowed[None], scores, -jnp.inf)
        highest_score = lax.optimization_barrier(jnp.max(scores, axis=-1))
        weights = jnp.exp(scores - highest_score[..., None])
        total = lax.optimization_barrier(jnp.sum(weights, axis=-1))
        summed = jnp.einsum('hqk,khd->qhd', weights.astype(jnp.bfloat16).astype(jnp.float32), values_wide)
        attended = (summed / jnp.transpose(total)[:, :, None]).astype(jnp.bfloat16)
        return (attended, highest_score + jnp.log(total))
    blocks_out, blocks_log = lax.map(attend, jnp.arange(TOKEN_SPAN // TOK_DEV, dtype=jnp.int32))
    attended = blocks_out.reshape(TOKEN_SPAN, MHEADS * VHEAD)
    log_total = jnp.transpose(blocks_log, (1, 0, 2)).reshape(MHEADS, TOKEN_SPAN)

    def heads(values):
        return values.astype(jnp.float32).reshape(TOKEN_SPAN, STATE_BRANCHES, BRANCH_CHANNELS)
    acceptance_tokens_flat = heads(matmul(normed, acceptance_projection).astype(jnp.bfloat16))
    state_address = heads(matmul(normed, state_address_projection).astype(jnp.bfloat16))
    state_content = heads(matmul(normed, state_content_projection).astype(jnp.bfloat16))
    decay_low = jnp.tanh(matmul(normed, fading_first_lowrank).astype(jnp.bfloat16).astype(jnp.float32)).astype(jnp.bfloat16)
    rate_logarithm = -jax.nn.softplus(-(fading_channel_bias + matmul(decay_low, fading_second_lowrank))) - 0.5
    decay_factor = jnp.exp(-jnp.exp(rate_logarithm).reshape(TOKEN_SPAN, STATE_BRANCHES, BRANCH_CHANNELS) * jnp.transpose(fading_speed_multiplier)[:, :, None] + jnp.transpose(fading_extra_exponent)[:, :, None])
    rate_low = matmul(normed, adaptation_first_lowrank).astype(jnp.bfloat16)
    learn = jax.nn.sigmoid(adaptation_channel_bias + matmul(rate_low, adaptation_second_lowrank)).reshape(TOKEN_SPAN, STATE_BRANCHES, BRANCH_CHANNELS)
    unit = state_address * lax.rsqrt(lax.optimization_barrier(jnp.sum(state_address * state_address, axis=-1, keepdims=True)) + 1e-06)
    start_state = jnp.zeros((STATE_BRANCHES, BRANCH_CHANNELS, BRANCH_CHANNELS), jnp.float32)
    _, read = lax.scan(recur, start_state, (decay_factor, unit, learn, state_content, state_address, acceptance_tokens_flat))
    center = lax.optimization_barrier(jnp.mean(read, axis=-1, keepdims=True))
    spread = lax.optimization_barrier(jnp.mean(jnp.square(read - center), axis=-1, keepdims=True))
    retrieved_rescaled = (read - center) * lax.rsqrt(spread + group_epsilon) * branch_rms_coefficients.reshape(STATE_BRANCHES, BRANCH_CHANNELS)
    present_token_term = lax.optimization_barrier(jnp.sum(acceptance_tokens_flat * state_address * present_token_coefficients, axis=-1, keepdims=True)) * state_content
    state_branch_result = (retrieved_rescaled + present_token_term).reshape(TOKEN_SPAN, STATE_BRANCHES * BRANCH_CHANNELS).astype(jnp.bfloat16)
    attn_cols = MHEADS * VHEAD // N_TP
    rec_cols = STATE_BRANCHES * BRANCH_CHANNELS // N_TP
    mixed = jnp.zeros((TOKEN_SPAN, D), jnp.float32)
    for group in range(N_TP):
        partial_sum = matmul(attended[:, group * attn_cols:(group + 1) * attn_cols], softmax_merge_projection[group * attn_cols:(group + 1) * attn_cols]) + matmul(state_branch_result[:, group * rec_cols:(group + 1) * rec_cols], state_merge_projection[group * rec_cols:(group + 1) * rec_cols])
        mixed = mixed + partial_sum.astype(jnp.bfloat16).astype(jnp.float32)
    return (mixed.astype(jnp.bfloat16), log_total)

def reference(layer_entering_vectors, entering_rms_coefficients, question_projection, compressing_projection, spinning_address_projection, compact_rms_coefficients, compact_to_plain_address, compact_to_content, question_rms_coefficients, address_rms_coefficients, acceptance_projection, state_address_projection, state_content_projection, fading_first_lowrank, fading_second_lowrank, fading_channel_bias, fading_speed_multiplier, fading_extra_exponent, adaptation_first_lowrank, adaptation_second_lowrank, adaptation_channel_bias, present_token_coefficients, branch_rms_coefficients, softmax_merge_projection, state_merge_projection):
    mixed_all = []
    logs_all = []
    for stream_position_entry in range(SEQS):
        solo_blended, solo_exponent_trace = solo_stream(layer_entering_vectors[stream_position_entry], entering_rms_coefficients, question_projection, compressing_projection, spinning_address_projection, compact_rms_coefficients, compact_to_plain_address, compact_to_content, question_rms_coefficients, address_rms_coefficients, acceptance_projection, state_address_projection, state_content_projection, fading_first_lowrank, fading_second_lowrank, fading_channel_bias, fading_speed_multiplier[stream_position_entry], fading_extra_exponent[stream_position_entry], adaptation_first_lowrank, adaptation_second_lowrank, adaptation_channel_bias, present_token_coefficients, branch_rms_coefficients, softmax_merge_projection, state_merge_projection)
        mixed_all.append(solo_blended)
        logs_all.append(solo_exponent_trace)
    return (jnp.stack(mixed_all), jnp.stack(logs_all))
```

```python
import jax
import jax.numpy as jnp
from jax import lax
from jax.experimental import pallas as pl
from jax.experimental.pallas import tpu as pltpu
from jax.sharding import PartitionSpec as P

NOPE = 64
ROPE = 32
VHEAD = 64
BRANCH_CHANNELS = 64
TOK_DEV = 256


norm_epsilon = 1e-06
group_epsilon = 0.00064
highest = lax.Precision.HIGHEST


def rms_rows(values, gain):
    floats = values.astype(jnp.float32)
    return (
        floats * lax.rsqrt(jnp.mean(floats * floats, axis=-1, keepdims=True) + norm_epsilon) * gain
    )


def rotate(values, positions):
    half = values.shape[-1] // 2
    inverse = 10000.0 ** (-jnp.arange(half, dtype=jnp.float32) / half)
    angle = positions.astype(jnp.float32)[:, None] * inverse[None, :]
    cosine = jnp.cos(angle)[:, None, :]
    sine = jnp.sin(angle)[:, None, :]
    first = values[..., :half]
    second = values[..., half:]
    return jnp.concatenate(
        [first * cosine - second * sine, second * cosine + first * sine], axis=-1
    )


def finish(stacked, gain, positions):
    normed = rms_rows(stacked, gain)
    return jnp.concatenate(
        [normed[..., :NOPE], rotate(normed[..., NOPE:], positions)], axis=-1
    ).astype(jnp.bfloat16)


def matmul(left, right):
    return jnp.dot(left, right, preferred_element_type=jnp.float32)


def mxu(left, right, contract):
    return lax.dot_general(
        left.astype(jnp.bfloat16),
        right.astype(jnp.bfloat16),
        ((contract[0], contract[1]), ((), ())),
        preferred_element_type=jnp.float32,
    )


plain = ((1,), (0,))
by_lanes = ((1,), (1,))
by_rows = ((0,), (0,))


def split_heads(values):
    width = values.shape[1]
    lane = lax.broadcasted_iota(jnp.int32, values.shape, 1)
    low = lane < width // 2
    return jnp.concatenate([jnp.where(low, values, 0.0), jnp.where(low, 0.0, values)], axis=0)


def head_sums(values):
    lane = lax.broadcasted_iota(jnp.int32, values.shape, 1)
    low = lane < values.shape[1] // 2
    first = jnp.sum(jnp.where(low, values, 0.0), axis=-1, keepdims=True)
    second = jnp.sum(jnp.where(low, 0.0, values), axis=-1, keepdims=True)
    return jnp.where(low, first, second)


def chunk_kernel(
    recept_ref, key_ref, value_ref, log_ref, learn_ref, free_ref, along_ref, state_ref
):
    rows, width = log_ref.shape
    size = BRANCH_CHANNELS
    chunks = rows // size
    row = lax.broadcasted_iota(jnp.int32, (size, width), 0)
    col = lax.broadcasted_iota(jnp.int32, (size, width), 1) & (size - 1)
    strict = row > col
    inclusive = row >= col
    tri = (
        lax.broadcasted_iota(jnp.int32, (size, size), 0)
        >= lax.broadcasted_iota(jnp.int32, (size, size), 1)
    ).astype(jnp.float32)
    wide_row = lax.broadcasted_iota(jnp.int32, (width, width), 0)
    wide_col = lax.broadcasted_iota(jnp.int32, (width, width), 1)
    same_head = (wide_row < size) == (wide_col < size)
    state = jnp.zeros((width, width), jnp.float32)
    along = (wide_row == wide_col).astype(jnp.float32)
    for chunk in range(chunks):
        here = pl.ds(chunk * size, size)
        log_decay = log_ref[here, :]
        cum = lax.dot_general(
            tri,
            log_decay,
            (((1,), (0,)), ((), ())),
            precision=highest,
            preferred_element_type=jnp.float32,
        )
        prev = cum - log_decay
        middle = cum[size // 2 - 1 : size // 2, :]
        end = cum[size - 1 : size, :]
        key = key_ref[here, :].astype(jnp.float32)
        value = value_ref[here, :].astype(jnp.float32)
        recept = recept_ref[here, :].astype(jnp.float32)
        unit = key * lax.rsqrt(head_sums(key * key) + 1e-06)
        remove = unit * learn_ref[here, :]
        grow = jnp.exp(middle - cum)
        left = jnp.concatenate([-unit * jnp.exp(prev - middle), recept * jnp.exp(cum - middle)], 0)
        right = jnp.concatenate([split_heads(remove * grow), split_heads(key * grow)], 0)
        pairs = mxu(left, right, by_lanes)
        remove_before = jnp.where(strict, pairs[:size, :width], 0.0)
        key_before = jnp.where(strict, pairs[:size, width:], 0.0)
        remove_upto = jnp.where(inclusive, pairs[size:, :width], 0.0)
        key_upto = jnp.where(inclusive, pairs[size:, width:], 0.0)
        inverse = (row == col).astype(jnp.float32) + jnp.where(
            (row >> 1) == (col >> 1), remove_before, 0.0
        )
        level = 1
        while (1 << level) < size:
            joins = ((row >> (level + 1)) == (col >> (level + 1))) & (
                (row >> level) != (col >> level)
            )
            inner = mxu(jnp.where(joins, remove_before, 0.0), split_heads(inverse), plain)
            inverse = inverse + mxu(inverse, split_heads(inner), plain)
            level += 1
        from_keys = mxu(
            jnp.concatenate([key_before, key_upto], 0), split_heads(value), plain
        )
        lead = mxu(
            inverse,
            jnp.concatenate(
                [split_heads(-unit * jnp.exp(prev)), split_heads(from_keys[:size])], 1
            ),
            plain,
        )
        lead_coef = lead[:, :width]
        lead_free = lead[:, width:]
        reads = mxu(
            remove_upto,
            jnp.concatenate([split_heads(lead_coef), split_heads(lead_free)], 1),
            plain,
        )
        coef = recept * jnp.exp(cum) + reads[:, :width]
        free = reads[:, width:] + from_keys[size:]
        tail = jnp.exp(end - cum)
        remove_tail = remove * tail
        step_map = jnp.where(same_head, mxu(lead_coef, remove_tail, by_rows), 0.0)
        step_add = jnp.where(
            same_head,
            mxu(
                jnp.concatenate([lead_free, value], 0),
                jnp.concatenate([remove_tail, key * tail], 0),
                by_rows,
            ),
            0.0,
        )
        both = jnp.concatenate([state, along], 0)
        read = mxu(coef, both, by_lanes)
        free_ref[here, :] = free + read[:, :width]
        along_ref[here, :] = read[:, width:]
        moved = both * jnp.exp(end) + mxu(both, step_map, plain)
        state = moved[:width] + step_add
        along = moved[width:]
    state_ref[0] = (along[:size] + along[size:]).astype(state_ref.dtype)
    state_ref[1] = (state[:size] + state[size:]).astype(state_ref.dtype)


def finish_kernel(
    place_ref, states_ref, free_ref, along_ref, recept_ref, key_ref, value_ref,
    present_ref, gain_ref, out_ref,
):
    place = place_ref[0]
    width = free_ref.shape[1]
    entering = jnp.zeros((width, width), jnp.float32)
    for other in range(states_ref.shape[0] - 1):
        transfer = split_heads(states_ref[other, 0].astype(jnp.float32))
        local = split_heads(states_ref[other, 1].astype(jnp.float32))
        advanced = mxu(entering, transfer, plain) + local
        entering = jnp.where(other < place, advanced, entering)
    read = free_ref[...] + mxu(along_ref[...], entering, by_lanes)
    center = head_sums(read) * (1.0 / BRANCH_CHANNELS)
    spread = head_sums(jnp.square(read - center)) * (1.0 / BRANCH_CHANNELS)
    rescaled = (read - center) * lax.rsqrt(spread + group_epsilon) * gain_ref[...]
    recept = recept_ref[...].astype(jnp.float32)
    key = key_ref[...].astype(jnp.float32)
    value = value_ref[...].astype(jnp.float32)
    own = head_sums(recept * key * present_ref[...]) * value
    out_ref[...] = (rescaled + own).astype(out_ref.dtype)


def recurrence(projected, offsets, log_decay, learn, present, gain):
    rows, total = log_decay.shape
    size = BRANCH_CHANNELS
    width = 2 * size
    groups = total // width

    def piece(offset):
        return pl.BlockSpec((rows, width), lambda i, first=offset // width: (0, first + i))

    spec = pl.BlockSpec((rows, width), lambda i: (0, i))
    vec = pl.BlockSpec((1, width), lambda i: (0, i))
    pieces = [piece(offset) for offset in offsets]
    free, along, states = pl.pallas_call(
        chunk_kernel,
        grid=(groups,),
        in_specs=pieces + [spec, spec],
        out_specs=[spec, spec, pl.BlockSpec((2, size, width), lambda i: (0, 0, i))],
        out_shape=[
            jax.ShapeDtypeStruct((rows, total), jnp.float32),
            jax.ShapeDtypeStruct((rows, total), jnp.float32),
            jax.ShapeDtypeStruct((2, size, total), jnp.bfloat16),
        ],
        cost_estimate=pl.CostEstimate(
            flops=groups * rows * width * width * 40, bytes_accessed=rows * total * 20, transcendentals=0
        ),
        name="chunks",
    )(projected, projected, projected, log_decay, learn)
    everyone = lax.all_gather(states, "sp", axis=0)
    place = lax.axis_index("sp").astype(jnp.int32).reshape(1)
    return pl.pallas_call(
        finish_kernel,
        grid=(groups,),
        in_specs=[
            pl.BlockSpec(memory_space=pltpu.SMEM),
            pl.BlockSpec((everyone.shape[0], 2, size, width), lambda i: (0, 0, 0, i)),
            spec,
            spec,
        ]
        + pieces
        + [vec, vec],
        out_specs=spec,
        out_shape=jax.ShapeDtypeStruct((rows, total), jnp.bfloat16),
        cost_estimate=pl.CostEstimate(
            flops=groups * rows * width * width * 8, bytes_accessed=rows * total * 16, transcendentals=0
        ),
        name="finish",
    )(place, everyone, free, along, projected, projected, projected, present, gain)


def shards(
    layer_entering_vectors,
    entering_rms_coefficients,
    question_projection,
    compressing_projection,
    spinning_address_projection,
    compact_rms_coefficients,
    compact_to_plain_address,
    compact_to_content,
    question_rms_coefficients,
    address_rms_coefficients,
    acceptance_projection,
    state_address_projection,
    state_content_projection,
    fading_first_lowrank,
    fading_second_lowrank,
    fading_channel_bias,
    fading_speed_multiplier,
    fading_extra_exponent,
    adaptation_first_lowrank,
    adaptation_second_lowrank,
    adaptation_channel_bias,
    present_token_coefficients,
    branch_rms_coefficients,
    softmax_merge_projection,
    state_merge_projection,
):
    recur_width = acceptance_projection.shape[1]
    recur_weights = lax.all_gather(
        jnp.concatenate(
            [acceptance_projection, state_address_projection, state_content_projection], axis=1
        ),
        "fs",
        axis=0,
        tiled=True,
    )
    attend_weights = lax.all_gather(
        jnp.concatenate(
            [compressing_projection, question_projection, spinning_address_projection], axis=1
        ),
        "fs",
        axis=0,
        tiled=True,
    )
    normed = rms_rows(
        lax.all_gather(layer_entering_vectors, "tp", axis=1, tiled=True)[0],
        entering_rms_coefficients,
    ).astype(jnp.bfloat16)
    decay_in = matmul(normed, fading_first_lowrank).astype(jnp.bfloat16)
    rate_low = matmul(normed, adaptation_first_lowrank).astype(jnp.bfloat16)
    recur_in = matmul(normed, recur_weights).astype(jnp.bfloat16)
    projected = matmul(normed, attend_weights).astype(jnp.bfloat16)
    latent_width = compressing_projection.shape[1]
    latent = projected[:, :latent_width]
    query = projected[:, latent_width : latent_width + question_projection.shape[1]]
    rope_key = projected[:, latent_width + question_projection.shape[1] :]
    row_count = projected.shape[0]
    attn_heads = compact_to_plain_address.shape[1] // NOPE
    qk_size = NOPE + ROPE
    own_positions = lax.axis_index("sp") * row_count + jnp.arange(row_count, dtype=jnp.int32)
    last_position = lax.axis_index("sp") * row_count + row_count - 1
    latent_normed = rms_rows(latent, compact_rms_coefficients).astype(jnp.bfloat16)
    query_ready = finish(
        query.reshape(row_count, attn_heads, qk_size), question_rms_coefficients, own_positions
    )
    scale = qk_size ** (-0.5)
    start_carry = (
        jnp.full((attn_heads, row_count), -jnp.inf, jnp.float32),
        jnp.zeros((attn_heads, row_count), jnp.float32),
        jnp.zeros((attn_heads, row_count, VHEAD), jnp.float32),
    )
    length_here = latent_normed.shape[0]
    key_nope = (
        matmul(latent_normed, compact_to_plain_address)
        .astype(jnp.bfloat16)
        .reshape(length_here, attn_heads, NOPE)
    )
    values_here = (
        matmul(latent_normed, compact_to_content)
        .astype(jnp.bfloat16)
        .reshape(length_here, attn_heads, VHEAD)
    )
    key_stack = jnp.concatenate(
        [key_nope, jnp.broadcast_to(rope_key[:, None, :], (length_here, attn_heads, ROPE))], axis=-1
    )
    key_ready = finish(key_stack, address_rms_coefficients, own_positions)
    carry = start_carry
    key_rows = lax.all_gather(key_ready, "sp", axis=0, tiled=True)
    length_here = key_rows.shape[0]
    block = TOK_DEV
    blocks = length_here // block
    keys_blocked = key_rows.reshape(blocks, block, attn_heads, qk_size)
    values_blocked = lax.all_gather(values_here, "sp", axis=0, tiled=True).reshape(
        blocks, block, attn_heads, VHEAD
    )

    def visit(state, inputs):
        key_block, value_block, index = inputs
        block_start = index * block

        def compute(running):
            running_max, running_total, running_sum = running
            scores = (
                jnp.einsum(
                    "qhd,khd->hqk", query_ready, key_block, preferred_element_type=jnp.float32
                )
                * scale
            )
            key_positions = block_start + jnp.arange(block, dtype=jnp.int32)
            allowed = key_positions[None, :] <= own_positions[:, None]
            scores = jnp.where(allowed[None], scores, -jnp.inf)
            new_max = jnp.maximum(running_max, jnp.max(scores, axis=-1))
            safe_max = jnp.where(jnp.isfinite(new_max), new_max, 0.0)
            weights = jnp.exp(scores - safe_max[..., None])
            factor = jnp.exp(running_max - safe_max)
            new_total = running_total * factor + jnp.sum(weights, axis=-1)
            new_sum = running_sum * factor[..., None] + jnp.einsum(
                "hqk,khd->hqd",
                weights.astype(jnp.bfloat16),
                value_block,
                preferred_element_type=jnp.float32,
            )
            return (new_max, new_total, new_sum)

        def keep(running):
            return running

        return (lax.cond(block_start > last_position, keep, compute, state), None)

    carry, _ = lax.scan(
        visit, carry, (keys_blocked, values_blocked, jnp.arange(blocks, dtype=jnp.int32))
    )
    final_max, final_total, final_sum = carry
    attended = (final_sum / final_total[..., None]).astype(jnp.bfloat16)
    attended = jnp.transpose(attended, (1, 0, 2)).reshape(row_count, attn_heads * VHEAD)
    log_total = final_max + jnp.log(final_total)
    recurrent_heads = fading_second_lowrank.shape[1] // BRANCH_CHANNELS

    decay_low = jnp.tanh(decay_in.astype(jnp.float32)).astype(jnp.bfloat16)
    rate_logarithm = (
        -jax.nn.softplus(-(fading_channel_bias + matmul(decay_low, fading_second_lowrank))) - 0.5
    )
    log_decay = (
        -jnp.exp(rate_logarithm).reshape(row_count, recurrent_heads, BRANCH_CHANNELS)
        * jnp.transpose(fading_speed_multiplier[0])[:, :, None]
        + jnp.transpose(fading_extra_exponent[0])[:, :, None]
    )
    learn = jax.nn.sigmoid(adaptation_channel_bias + matmul(rate_low, adaptation_second_lowrank))
    state_branch_result = recurrence(
        recur_in,
        (0, recur_width, 2 * recur_width),
        log_decay.reshape(row_count, recur_width),
        learn,
        present_token_coefficients.reshape(1, recur_width),
        branch_rms_coefficients.reshape(1, recur_width),
    )
    out_attn_full, out_rec_full = (
        lax.all_gather(softmax_merge_projection, "fs", axis=1, tiled=True),
        lax.all_gather(state_merge_projection, "fs", axis=1, tiled=True),
    )
    mixed = lax.psum_scatter(
        (matmul(attended, out_attn_full) + matmul(state_branch_result, out_rec_full)).astype(
            jnp.bfloat16
        ),
        "tp",
        scatter_dimension=0,
        tiled=True,
    )
    return (mixed[None], log_total[None])


def solution(mesh):
    placed = (
        P("fs", ("sp", "tp"), None),
        P(),
        P("fs", "tp"),
        P("fs", None),
        P("fs", None),
        P(),
        P(None, "tp"),
        P(None, "tp"),
        P(),
        P(),
        P("fs", "tp"),
        P("fs", "tp"),
        P("fs", "tp"),
        P(),
        P(None, "tp"),
        P("tp"),
        P("fs", "tp", "sp"),
        P("fs", "tp", "sp"),
        P(),
        P(None, "tp"),
        P("tp"),
        P("tp", None),
        P("tp"),
        P("tp", "fs"),
        P("tp", "fs"),
    )
    return jax.shard_map(
        shards,
        mesh=mesh,
        in_specs=placed,
        out_specs=(P("fs", ("sp", "tp"), None), P("fs", "tp", "sp")),
        check_vma=False,
    )
```

```python
import jax
import jax.numpy as jnp
from jax import lax
from jax.experimental import pallas as pl
from jax.experimental.pallas import tpu as pltpu
from jax.sharding import PartitionSpec as P

NOPE = 64
ROPE = 32
VHEAD = 64
BRANCH_CHANNELS = 64
TOK_DEV = 256


norm_epsilon = 1e-06
group_epsilon = 0.00064
highest = lax.Precision.HIGHEST


def rms_rows(values, gain):
    floats = values.astype(jnp.float32)
    return (
        floats * lax.rsqrt(jnp.mean(floats * floats, axis=-1, keepdims=True) + norm_epsilon) * gain
    )


def rotate(values, positions):
    half = values.shape[-1] // 2
    inverse = 10000.0 ** (-jnp.arange(half, dtype=jnp.float32) / half)
    angle = positions.astype(jnp.float32)[:, None] * inverse[None, :]
    cosine = jnp.cos(angle)[:, None, :]
    sine = jnp.sin(angle)[:, None, :]
    first = values[..., :half]
    second = values[..., half:]
    return jnp.concatenate(
        [first * cosine - second * sine, second * cosine + first * sine], axis=-1
    )


def finish(stacked, gain, positions):
    normed = rms_rows(stacked, gain)
    return jnp.concatenate(
        [normed[..., :NOPE], rotate(normed[..., NOPE:], positions)], axis=-1
    ).astype(jnp.bfloat16)


def matmul(left, right):
    return jnp.dot(left, right, preferred_element_type=jnp.float32)


def mxu(left, right, contract):
    return lax.dot_general(
        left.astype(jnp.bfloat16),
        right.astype(jnp.bfloat16),
        ((contract[0], contract[1]), ((), ())),
        preferred_element_type=jnp.float32,
    )


plain = ((1,), (0,))
by_lanes = ((1,), (1,))
by_rows = ((0,), (0,))


def split_heads(values):
    width = values.shape[1]
    lane = lax.broadcasted_iota(jnp.int32, values.shape, 1)
    low = lane < width // 2
    return jnp.concatenate([jnp.where(low, values, 0.0), jnp.where(low, 0.0, values)], axis=0)


def head_sums(values):
    lane = lax.broadcasted_iota(jnp.int32, values.shape, 1)
    low = lane < values.shape[1] // 2
    first = jnp.sum(jnp.where(low, values, 0.0), axis=-1, keepdims=True)
    second = jnp.sum(jnp.where(low, 0.0, values), axis=-1, keepdims=True)
    return jnp.where(low, first, second)


def chunk_kernel(
    recept_ref, key_ref, value_ref, log_ref, learn_ref, free_ref, along_ref, state_ref
):
    rows, width = log_ref.shape
    size = BRANCH_CHANNELS
    chunks = rows // size
    row = lax.broadcasted_iota(jnp.int32, (size, width), 0)
    col = lax.broadcasted_iota(jnp.int32, (size, width), 1) & (size - 1)
    strict = row > col
    inclusive = row >= col
    tri = (
        lax.broadcasted_iota(jnp.int32, (size, size), 0)
        >= lax.broadcasted_iota(jnp.int32, (size, size), 1)
    ).astype(jnp.float32)
    wide_row = lax.broadcasted_iota(jnp.int32, (width, width), 0)
    wide_col = lax.broadcasted_iota(jnp.int32, (width, width), 1)
    same_head = (wide_row < size) == (wide_col < size)
    state = jnp.zeros((width, width), jnp.float32)
    along = (wide_row == wide_col).astype(jnp.float32)
    for chunk in range(chunks):
        here = pl.ds(chunk * size, size)
        log_decay = log_ref[here, :]
        cum = lax.dot_general(
            tri,
            log_decay,
            (((1,), (0,)), ((), ())),
            precision=highest,
            preferred_element_type=jnp.float32,
        )
        prev = cum - log_decay
        middle = cum[size // 2 - 1 : size // 2, :]
        end = cum[size - 1 : size, :]
        key = key_ref[here, :].astype(jnp.float32)
        value = value_ref[here, :].astype(jnp.float32)
        recept = recept_ref[here, :].astype(jnp.float32)
        unit = key * lax.rsqrt(head_sums(key * key) + 1e-06)
        remove = unit * learn_ref[here, :]
        grow = jnp.exp(middle - cum)
        left = jnp.concatenate([-unit * jnp.exp(prev - middle), recept * jnp.exp(cum - middle)], 0)
        right = jnp.concatenate([split_heads(remove * grow), split_heads(key * grow)], 0)
        pairs = mxu(left, right, by_lanes)
        remove_before = jnp.where(strict, pairs[:size, :width], 0.0)
        key_before = jnp.where(strict, pairs[:size, width:], 0.0)
        remove_upto = jnp.where(inclusive, pairs[size:, :width], 0.0)
        key_upto = jnp.where(inclusive, pairs[size:, width:], 0.0)
        inverse = (row == col).astype(jnp.float32) + jnp.where(
            (row >> 1) == (col >> 1), remove_before, 0.0
        )
        level = 1
        while (1 << level) < size:
            joins = ((row >> (level + 1)) == (col >> (level + 1))) & (
                (row >> level) != (col >> level)
            )
            inner = mxu(jnp.where(joins, remove_before, 0.0), split_heads(inverse), plain)
            inverse = inverse + mxu(inverse, split_heads(inner), plain)
            level += 1
        from_keys = mxu(
            jnp.concatenate([key_before, key_upto], 0), split_heads(value), plain
        )
        lead = mxu(
            inverse,
            jnp.concatenate(
                [split_heads(-unit * jnp.exp(prev)), split_heads(from_keys[:size])], 1
            ),
            plain,
        )
        lead_coef = lead[:, :width]
        lead_free = lead[:, width:]
        reads = mxu(
            remove_upto,
            jnp.concatenate([split_heads(lead_coef), split_heads(lead_free)], 1),
            plain,
        )
        coef = recept * jnp.exp(cum) + reads[:, :width]
        free = reads[:, width:] + from_keys[size:]
        tail = jnp.exp(end - cum)
        remove_tail = remove * tail
        step_map = jnp.where(same_head, mxu(lead_coef, remove_tail, by_rows), 0.0)
        step_add = jnp.where(
            same_head,
            mxu(
                jnp.concatenate([lead_free, value], 0),
                jnp.concatenate([remove_tail, key * tail], 0),
                by_rows,
            ),
            0.0,
        )
        both = jnp.concatenate([state, along], 0)
        read = mxu(coef, both, by_lanes)
        free_ref[here, :] = free + read[:, :width]
        along_ref[here, :] = read[:, width:]
        moved = both * jnp.exp(end) + mxu(both, step_map, plain)
        state = moved[:width] + step_add
        along = moved[width:]
    state_ref[0] = (along[:size] + along[size:]).astype(state_ref.dtype)
    state_ref[1] = (state[:size] + state[size:]).astype(state_ref.dtype)


def finish_kernel(
    place_ref, states_ref, free_ref, along_ref, recept_ref, key_ref, value_ref,
    present_ref, gain_ref, out_ref,
):
    place = place_ref[0]
    width = free_ref.shape[1]
    entering = jnp.zeros((width, width), jnp.float32)
    for other in range(states_ref.shape[0] - 1):
        transfer = split_heads(states_ref[other, 0].astype(jnp.float32))
        local = split_heads(states_ref[other, 1].astype(jnp.float32))
        advanced = mxu(entering, transfer, plain) + local
        entering = jnp.where(other < place, advanced, entering)
    read = free_ref[...] + mxu(along_ref[...], entering, by_lanes)
    center = head_sums(read) * (1.0 / BRANCH_CHANNELS)
    spread = head_sums(jnp.square(read - center)) * (1.0 / BRANCH_CHANNELS)
    rescaled = (read - center) * lax.rsqrt(spread + group_epsilon) * gain_ref[...]
    recept = recept_ref[...].astype(jnp.float32)
    key = key_ref[...].astype(jnp.float32)
    value = value_ref[...].astype(jnp.float32)
    own = head_sums(recept * key * present_ref[...]) * value
    out_ref[...] = (rescaled + own).astype(out_ref.dtype)


def exchange(block, axis, distance):
    route = [(i, i ^ distance) for i in range(lax.axis_size(axis))]
    return lax.ppermute(block, axis, route)


def assemble(blocks, axis, dimension):
    place = lax.axis_index(axis)
    length = blocks[0].shape[dimension]
    shape = list(blocks[0].shape)
    shape[dimension] = length * len(blocks)
    whole = jnp.zeros(shape, blocks[0].dtype)
    for distance, block in enumerate(blocks):
        whole = lax.dynamic_update_slice_in_dim(
            whole, block, (place ^ distance) * length, dimension
        )
    return whole


def gather_by(block, axis, dimension):
    blocks = [block] + [exchange(block, axis, d) for d in range(1, lax.axis_size(axis))]
    return assemble(blocks, axis, dimension)


def returned(rows, weights):
    partial = [matmul(piece, weights).astype(jnp.bfloat16) for piece in rows]
    total = partial[0].astype(jnp.float32)
    for distance in range(1, len(partial)):
        total = total + exchange(partial[distance], "fs", distance).astype(jnp.float32)
    return total.astype(jnp.bfloat16)


def recurrence(projected, offsets, log_decay, learn, present, gain):
    rows, total = log_decay.shape
    size = BRANCH_CHANNELS
    width = 2 * size
    groups = total // width

    def piece(offset):
        return pl.BlockSpec((rows, width), lambda i, first=offset // width: (0, first + i))

    spec = pl.BlockSpec((rows, width), lambda i: (0, i))
    vec = pl.BlockSpec((1, width), lambda i: (0, i))
    pieces = [piece(offset) for offset in offsets]
    free, along, states = pl.pallas_call(
        chunk_kernel,
        grid=(groups,),
        in_specs=pieces + [spec, spec],
        out_specs=[spec, spec, pl.BlockSpec((2, size, width), lambda i: (0, 0, i))],
        out_shape=[
            jax.ShapeDtypeStruct((rows, total), jnp.float32),
            jax.ShapeDtypeStruct((rows, total), jnp.float32),
            jax.ShapeDtypeStruct((2, size, total), jnp.bfloat16),
        ],
        cost_estimate=pl.CostEstimate(
            flops=groups * rows * width * width * 40, bytes_accessed=rows * total * 20, transcendentals=0
        ),
        name="chunks",
    )(projected, projected, projected, log_decay, learn)
    everyone = lax.all_gather(states, "sp", axis=0)
    place = lax.axis_index("sp").astype(jnp.int32).reshape(1)
    return pl.pallas_call(
        finish_kernel,
        grid=(groups,),
        in_specs=[
            pl.BlockSpec(memory_space=pltpu.SMEM),
            pl.BlockSpec((everyone.shape[0], 2, size, width), lambda i: (0, 0, 0, i)),
            spec,
            spec,
        ]
        + pieces
        + [vec, vec],
        out_specs=spec,
        out_shape=jax.ShapeDtypeStruct((rows, total), jnp.bfloat16),
        cost_estimate=pl.CostEstimate(
            flops=groups * rows * width * width * 8, bytes_accessed=rows * total * 16, transcendentals=0
        ),
        name="finish",
    )(place, everyone, free, along, projected, projected, projected, present, gain)


def shards(
    layer_entering_vectors,
    entering_rms_coefficients,
    question_projection,
    compressing_projection,
    spinning_address_projection,
    compact_rms_coefficients,
    compact_to_plain_address,
    compact_to_content,
    question_rms_coefficients,
    address_rms_coefficients,
    acceptance_projection,
    state_address_projection,
    state_content_projection,
    fading_first_lowrank,
    fading_second_lowrank,
    fading_channel_bias,
    fading_speed_multiplier,
    fading_extra_exponent,
    adaptation_first_lowrank,
    adaptation_second_lowrank,
    adaptation_channel_bias,
    present_token_coefficients,
    branch_rms_coefficients,
    softmax_merge_projection,
    state_merge_projection,
):
    recur_width = acceptance_projection.shape[1]
    group = lax.axis_size("fs")
    normed = rms_rows(layer_entering_vectors[0], entering_rms_coefficients).astype(jnp.bfloat16)
    features = acceptance_projection.shape[0]
    own = lax.axis_index("fs")
    parts = []
    for distance in range(group):
        part = lax.dynamic_slice_in_dim(normed, (own ^ distance) * features, features, 1)
        parts.append(part if distance == 0 else exchange(part, "fs", distance))
    gathered = gather_by(jnp.stack(parts), "tp", 1)
    rows = [gathered[distance] for distance in range(group)]
    recur_in = returned(
        rows,
        jnp.concatenate(
            [acceptance_projection, state_address_projection, state_content_projection], axis=1
        ),
    )
    projected = returned(
        rows,
        jnp.concatenate(
            [compressing_projection, question_projection, spinning_address_projection], axis=1
        ),
    )
    lows = gather_by(
        matmul(
            normed, jnp.concatenate([fading_first_lowrank, adaptation_first_lowrank], axis=1)
        ).astype(jnp.bfloat16),
        "tp",
        0,
    )
    decay_in = lows[:, : fading_first_lowrank.shape[1]]
    rate_low = lows[:, fading_first_lowrank.shape[1] :]
    latent_width = compressing_projection.shape[1]
    latent = projected[:, :latent_width]
    query = projected[:, latent_width : latent_width + question_projection.shape[1]]
    rope_key = projected[:, latent_width + question_projection.shape[1] :]
    row_count = projected.shape[0]
    attn_heads = compact_to_plain_address.shape[1] // NOPE
    qk_size = NOPE + ROPE
    own_positions = lax.axis_index("sp") * row_count + jnp.arange(row_count, dtype=jnp.int32)
    last_position = lax.axis_index("sp") * row_count + row_count - 1
    latent_normed = rms_rows(latent, compact_rms_coefficients).astype(jnp.bfloat16)
    query_ready = finish(
        query.reshape(row_count, attn_heads, qk_size), question_rms_coefficients, own_positions
    )
    scale = qk_size ** (-0.5)
    start_carry = (
        jnp.full((attn_heads, row_count), -jnp.inf, jnp.float32),
        jnp.zeros((attn_heads, row_count), jnp.float32),
        jnp.zeros((attn_heads, row_count, VHEAD), jnp.float32),
    )
    length_here = latent_normed.shape[0]
    key_nope = (
        matmul(latent_normed, compact_to_plain_address)
        .astype(jnp.bfloat16)
        .reshape(length_here, attn_heads, NOPE)
    )
    values_here = (
        matmul(latent_normed, compact_to_content)
        .astype(jnp.bfloat16)
        .reshape(length_here, attn_heads, VHEAD)
    )
    key_stack = jnp.concatenate(
        [key_nope, jnp.broadcast_to(rope_key[:, None, :], (length_here, attn_heads, ROPE))], axis=-1
    )
    key_ready = finish(key_stack, address_rms_coefficients, own_positions)
    carry = start_carry
    key_rows = lax.all_gather(key_ready, "sp", axis=0, tiled=True)
    length_here = key_rows.shape[0]
    block = TOK_DEV
    blocks = length_here // block
    keys_blocked = key_rows.reshape(blocks, block, attn_heads, qk_size)
    values_blocked = lax.all_gather(values_here, "sp", axis=0, tiled=True).reshape(
        blocks, block, attn_heads, VHEAD
    )

    def visit(state, inputs):
        key_block, value_block, index = inputs
        block_start = index * block

        def compute(running):
            running_max, running_total, running_sum = running
            scores = (
                jnp.einsum(
                    "qhd,khd->hqk", query_ready, key_block, preferred_element_type=jnp.float32
                )
                * scale
            )
            key_positions = block_start + jnp.arange(block, dtype=jnp.int32)
            allowed = key_positions[None, :] <= own_positions[:, None]
            scores = jnp.where(allowed[None], scores, -jnp.inf)
            new_max = jnp.maximum(running_max, jnp.max(scores, axis=-1))
            safe_max = jnp.where(jnp.isfinite(new_max), new_max, 0.0)
            weights = jnp.exp(scores - safe_max[..., None])
            factor = jnp.exp(running_max - safe_max)
            new_total = running_total * factor + jnp.sum(weights, axis=-1)
            new_sum = running_sum * factor[..., None] + jnp.einsum(
                "hqk,khd->hqd",
                weights.astype(jnp.bfloat16),
                value_block,
                preferred_element_type=jnp.float32,
            )
            return (new_max, new_total, new_sum)

        def keep(running):
            return running

        return (lax.cond(block_start > last_position, keep, compute, state), None)

    carry, _ = lax.scan(
        visit, carry, (keys_blocked, values_blocked, jnp.arange(blocks, dtype=jnp.int32))
    )
    final_max, final_total, final_sum = carry
    attended = (final_sum / final_total[..., None]).astype(jnp.bfloat16)
    attended = jnp.transpose(attended, (1, 0, 2)).reshape(row_count, attn_heads * VHEAD)
    log_total = final_max + jnp.log(final_total)
    recurrent_heads = fading_second_lowrank.shape[1] // BRANCH_CHANNELS

    decay_low = jnp.tanh(decay_in.astype(jnp.float32)).astype(jnp.bfloat16)
    rate_logarithm = (
        -jax.nn.softplus(-(fading_channel_bias + matmul(decay_low, fading_second_lowrank))) - 0.5
    )
    log_decay = (
        -jnp.exp(rate_logarithm).reshape(row_count, recurrent_heads, BRANCH_CHANNELS)
        * jnp.transpose(fading_speed_multiplier[0])[:, :, None]
        + jnp.transpose(fading_extra_exponent[0])[:, :, None]
    )
    learn = jax.nn.sigmoid(adaptation_channel_bias + matmul(rate_low, adaptation_second_lowrank))
    state_branch_result = recurrence(
        recur_in,
        (0, recur_width, 2 * recur_width),
        log_decay.reshape(row_count, recur_width),
        learn,
        present_token_coefficients.reshape(1, recur_width),
        branch_rms_coefficients.reshape(1, recur_width),
    )
    attn_out, rec_out, _ = lax.optimization_barrier(
        (softmax_merge_projection, state_merge_projection, recur_in)
    )
    columns = []
    for distance in range(group):
        attn_block, rec_block = attn_out, rec_out
        if distance:
            attn_block = exchange(attn_out, "fs", distance)
            rec_block = exchange(rec_out, "fs", distance)
        columns.append(
            (matmul(attended, attn_block) + matmul(state_branch_result, rec_block)).astype(
                jnp.bfloat16
            )
        )
    shared = assemble(columns, "fs", 1)
    pair = lax.axis_index("tp")
    sharers = lax.axis_size("tp")
    kept = row_count // sharers
    total = None
    for distance in range(sharers):
        part = lax.dynamic_slice_in_dim(shared, (pair ^ distance) * kept, kept, 0)
        if distance:
            part = exchange(part, "tp", distance)
        part = part.astype(jnp.float32)
        total = part if total is None else total + part
    mixed = total.astype(jnp.bfloat16)
    return (mixed[None], log_total[None])


def solution(mesh):
    placed = (
        P("fs", ("sp", "tp"), None),
        P(),
        P("fs", "tp"),
        P("fs", None),
        P("fs", None),
        P(),
        P(None, "tp"),
        P(None, "tp"),
        P(),
        P(),
        P("fs", "tp"),
        P("fs", "tp"),
        P("fs", "tp"),
        P(),
        P(None, "tp"),
        P("tp"),
        P("fs", "tp", "sp"),
        P("fs", "tp", "sp"),
        P(),
        P(None, "tp"),
        P("tp"),
        P("tp", None),
        P("tp"),
        P("tp", "fs"),
        P("tp", "fs"),
    )
    return jax.shard_map(
        shards,
        mesh=mesh,
        in_specs=placed,
        out_specs=(P("fs", ("sp", "tp"), None), P("fs", "tp", "sp")),
        check_vma=False,
    )
```
